32 devices in a mesh: sp: 8 (over z, x), dp: 4 (over y, core).
Axes of the slice: x: 2, y: 2, z: 4, core: 2. Of those that a mesh axis runs over, the one named last changes fastest.
Arguments:
- resid: bfloat16 [4, 2048, 2048], P('dp', 'sp'), may hold values from -4 to 4
- query: bfloat16 [4, 2048, 2048], P('dp', 'sp'), may hold values from -6 to 6
- keys: bfloat16 [4, 2048, 512], P('dp', 'sp'), may hold values from -6 to 6
- values: bfloat16 [4, 2048, 512], P('dp', 'sp'), may hold values from -6 to 6
- q_gain: float32 [128], replicated, may hold values from 0.7 to 5
- k_gain: float32 [128], replicated, may hold values from 0.7 to 5
- out_weight: bfloat16 [2048, 2048], P('dp'), may hold values from -0.5 to 0.5
- norm_gain: float32 [2048], replicated, may hold values from 0.1 to 1.9
- route_ids: int32 [4, 2048, 2], P('dp', 'sp'), may hold values from 0 to 31, all different within a row; in each aligned block of 256 rows (0 to 255, 256 to 511, ..., all dimensions but the last counted through in order) at most 24 rows name the same one
- route_weight: float32 [4, 2048, 2], P('dp', 'sp'), may hold values from 0.2 to 1
- expert_gate: bfloat16 [32, 2048, 1024], P(('sp', 'dp')), may hold values from -0.125 to 0.125
- expert_up: bfloat16 [32, 2048, 1024], P(('sp', 'dp')), may hold values from -0.125 to 0.125
- expert_down: bfloat16 [32, 1024, 2048], P(('sp', 'dp')), may hold values from -0.1875 to 0.1875
Outputs:
- layer_out: bfloat16 [4, 2048, 2048], P('dp', 'sp')
The draws below stay inside these ranges and needn't reach their ends.
Inputs may be any that keep to these rules, and one draw needn't show every extreme that they name: `route_ids`: each row names 2 different experts. In the rows of one device no expert is named more than 24 times, and in some devices some expert is named exactly 24 times.
All inputs are finite; a program needn't handle non-finite values.
Results may differ from the reference program's by a relative error of at most 0.0095.
The reference program's roundings to bfloat16 on the way count: a program that leaves them out, or rounds other values in their place, can miss the bound.
Values may be sent and summed in bfloat16 or wider, within the bound.
A program may use at most 128 MiB of HBM per device.

```python
import math
import jax
import jax.numpy as jnp
import numpy as np
from jax import lax

D = 2048
QH = 16
KVH = 4
HD = 128
FE = 1024
TOP = 2
GRID_W = 64
TOK_DEV = 256
LEN = 2048
SEQS = 4
EXPERTS = 32
CAP = 24
N_SP = 8
N_DP = 4


def drawn_keys(key):
    return jnp.clip(jax.random.normal(jax.random.fold_in(key, 31), (SEQS, LEN, KVH * HD), jnp.float32), -6.0, 6.0)


def draw_keys(key, part):
    return drawn_keys(key).astype(jnp.bfloat16)


def draw_query(key, part):
    base = jnp.clip(jax.random.normal(jax.random.fold_in(key, 32), (SEQS, LEN, QH * HD), jnp.float32), -6.0, 6.0)
    return base.astype(jnp.bfloat16)


def gain_draw(key, salt):
    return jax.random.uniform(jax.random.fold_in(key, salt), (HD,), jnp.float32, 0.7, 1.6)


def draw_q_gain(key, part):
    return gain_draw(key, 41)


def draw_k_gain(key, part):
    return gain_draw(key, 42)


def block_levels(key, shape, split, low, high):
    factor_of, own = 1.0, jax.random.fold_in(key, 6)
    for position, parts in split:
        heights = jnp.exp(jax.random.uniform(jax.random.fold_in(own, position), (parts,), jnp.float32, low / len(split), high / len(split)))
        factor_of = factor_of * jnp.repeat(heights, shape[position] // parts).reshape([-1 if axis == position else 1 for axis in range(len(shape))])
    return factor_of


def routed_block(rng, own, number, rows, count, top, limit, slope):
    order = jax.random.permutation(rng, count)
    packed, ordinary = shares(count, rows * top, limit, slope, True), shares(count, rows * top, limit, slope, False)
    places = jnp.arange(count)

    def named(sizes, turn):
        used = int((sizes > 0).sum())
        fixed = max(1, used // 4)
        moved = fixed + (places - fixed + turn * (used - fixed)) % max(1, count - fixed)
        return jnp.zeros((count,), jnp.int32).at[order[jnp.where(places < fixed, places, moved)]].set(jnp.asarray(sizes, jnp.int32))

    sizes = jnp.where(number % 4 == 0, named(packed, number // 4), named(ordinary, number - number // 4 - 1))
    mixed = jax.random.permutation(jax.random.fold_in(own, 3), count)
    giver, sink = mixed[0:count // 2 * 2:2], mixed[1:count // 2 * 2:2]
    room = jnp.minimum(sizes[giver] - 1, limit - sizes[sink]) // 2
    room = jnp.where((giver == order[0]) | (sink == order[0]) | (sizes[sink] == 0), 0, jnp.maximum(room, 0))
    moved = jax.random.randint(jax.random.fold_in(own, 4), (count // 2,), 0, 1 << 20) % (room + 1)
    sizes = sizes.at[giver].add(-moved).at[sink].add(moved)
    labels = jnp.searchsorted(jnp.cumsum(sizes), jnp.arange(rows * top), side="right").astype(jnp.int32)
    grid = labels.reshape(top, rows).T
    grid = grid[jax.random.permutation(jax.random.fold_in(own, 1), rows)]
    turn = jax.random.randint(jax.random.fold_in(own, 2), (rows, 1), 0, top)
    return jnp.take_along_axis(grid, (jnp.arange(top)[None, :] + turn) % top, axis=1)


def shares(amount, total, bound, lean, full):
    weights = [(1 << 20) // math.isqrt(rank ** lean) + 1 for rank in range(1, amount + 1)]
    largest = bound if full else min(bound, max(-(-total // amount), total * weights[0] // sum(weights)))
    least = 1 if total - largest >= amount - 1 else 0
    given, spare = [largest] + [least] * (amount - 1), total - largest - least * (amount - 1)
    while spare > 0:
        candidates = [i for i in range(1, amount) if given[i] < largest] or [i for i in range(1, amount) if given[i] < bound]
        whole, left = sum([weights[i] for i in candidates]), spare
        for i in candidates:
            extra = min(bound - given[i], max(1, left * weights[i] // whole), spare)
            given[i] = given[i] + extra
            spare = spare - extra
    return np.array(given)


def scatter_about(rng, dims, width, most, split=(), kind=jnp.bfloat16):
    array = jax.random.normal(rng, dims, jnp.float32) * width
    if len(split) > 0:
        array = block_levels(rng, dims, split, -0.22, 0.18) * array
    return jnp.clip(array, min=-most, max=most).astype(kind)


def setup_inputs(seed: int = 0) -> dict:
    seeds = jax.random.split(jax.random.key(seed), 14)
    resid = scatter_about(seeds[0], (SEQS, LEN, D), 0.5, 4.0, ((0, 4), (1, 8)))
    query = draw_query(jax.random.fold_in(seeds[13], 71), 0)
    keys = draw_keys(jax.random.fold_in(seeds[13], 71), 0)
    values = scatter_about(seeds[3], (SEQS, LEN, KVH * HD), 1.0, 6.0, ((0, 4), (1, 8)))
    q_gain = draw_q_gain(jax.random.fold_in(seeds[13], 71), 0)
    k_gain = draw_k_gain(jax.random.fold_in(seeds[13], 71), 0)
    out_weight = scatter_about(seeds[6], (QH * HD, D), HD ** -0.5, 0.5, ((0, 4),))
    norm_gain = jnp.clip(1.0 + 0.18 * jax.random.normal(seeds[7], (D,), jnp.float32), 0.1, 1.9)
    route_ids_keys = jax.random.split(jax.random.fold_in(seeds[8], 1), SEQS * LEN // TOK_DEV)
    route_ids_turns = jax.random.permutation(jax.random.fold_in(seeds[8], 3), SEQS * LEN // TOK_DEV)
    route_ids = jax.vmap(lambda own, number: routed_block(jax.random.fold_in(seeds[8], 2), own, number, TOK_DEV, EXPERTS, TOP, CAP, 2))(route_ids_keys, route_ids_turns).reshape((SEQS, LEN, TOP))
    route_weight = jnp.clip(0.2 + 0.8 * jax.random.uniform(seeds[9], (SEQS, LEN, TOP), jnp.float32) ** block_levels(seeds[9], (SEQS, LEN, TOP), ((0, 4), (1, 8)), -0.2, 0.2), 0.2, 1.0)
    expert_gate = scatter_about(seeds[10], (EXPERTS, D, FE), D ** -0.5, 0.125, ((0, 32),))
    expert_up = scatter_about(seeds[11], (EXPERTS, D, FE), D ** -0.5, 0.125, ((0, 32),))
    expert_down = scatter_about(seeds[12], (EXPERTS, FE, D), FE ** -0.5, 0.1875, ((0, 32),))
    return {"resid": resid, "query": query, "keys": keys, "values": values, "q_gain": q_gain, "k_gain": k_gain, "out_weight": out_weight, "norm_gain": norm_gain, "route_ids": route_ids, "route_weight": route_weight, "expert_gate": expert_gate, "expert_up": expert_up, "expert_down": expert_down}


EPSILON = 1e-06
THETA = 10000.0
LIMIT = 7.0
SLOPE = 1.702

def turn_half(matrix, places):
    half_width = matrix.shape[-1] // 2
    inverse = THETA ** (-jnp.arange(half_width, dtype=jnp.float32) / half_width)
    angles = places.astype(jnp.float32)[:, None] * inverse[None, :]
    cosine = jnp.cos(angles)[:, None, :]
    sine_part = jnp.sin(angles)[:, None, :]
    leading = matrix[..., :half_width]
    second = matrix[..., half_width:]
    return jnp.concatenate([leading * cosine - second * sine_part, second * cosine + leading * sine_part], axis=-1)

def prepare(projected_rows, gain_vector, head_count, places):
    matrix = projected_rows.astype(jnp.float32).reshape(projected_rows.shape[0], head_count, -1)
    matrix = matrix * lax.rsqrt(lax.optimization_barrier(jnp.mean(matrix * matrix, axis=-1, keepdims=True)) + EPSILON) * gain_vector
    middle = matrix.shape[-1] // 2
    turned = jnp.concatenate([turn_half(matrix[..., :middle], places // GRID_W), turn_half(matrix[..., middle:], places % GRID_W)], axis=-1)
    return turned.astype(jnp.bfloat16)

def attend(head_query, head_key, head_value):
    length, local_heads, head_dim = head_query.shape
    local_kv = head_key.shape[1]
    group_size = local_heads // local_kv
    block_rows = min(512, length)
    scaling = head_dim ** (-0.5)
    query_blocks = head_query.reshape(length // block_rows, block_rows, local_kv, group_size, head_dim)
    key_wide = head_key.astype(jnp.float32)
    value_wide = head_value.astype(jnp.float32)

    def one_block(query_block):
        scores = jnp.einsum('qkgd,skd->kgqs', query_block.astype(jnp.float32), key_wide) * scaling
        lifted = jnp.exp(scores - lax.optimization_barrier(jnp.max(scores, axis=-1, keepdims=True)))
        attn_weights = (lifted / lax.optimization_barrier(jnp.sum(lifted, axis=-1, keepdims=True))).astype(jnp.bfloat16)
        return jnp.einsum('kgqs,skd->qkgd', attn_weights.astype(jnp.float32), value_wide).astype(jnp.bfloat16)
    return lax.map(one_block, query_blocks).reshape(length, local_heads, head_dim)

def apply_expert(batch, gate_matrix, up_matrix, down_matrix):
    flat_rows = batch.reshape(-1, batch.shape[-1])
    gated = jnp.minimum(jnp.dot(flat_rows, gate_matrix, preferred_element_type=jnp.float32), LIMIT)
    linear = jnp.clip(jnp.dot(flat_rows, up_matrix, preferred_element_type=jnp.float32), -LIMIT, LIMIT)
    active = (gated * jax.nn.sigmoid(SLOPE * gated) * (linear + 1.0)).astype(jnp.bfloat16)
    return jnp.dot(active, down_matrix, preferred_element_type=jnp.float32).astype(jnp.bfloat16).reshape(batch.shape)

def block_tables(block_ids, block_weights):
    chosen = block_ids.reshape(-1)
    onehot = (chosen[:, None] == jnp.arange(EXPERTS, dtype=jnp.int32)[None, :]).astype(jnp.int32)
    earlier = lax.optimization_barrier(jnp.sum((jnp.cumsum(onehot, axis=0) - onehot) * onehot, axis=1))
    target = (chosen * CAP + earlier).astype(jnp.int32)
    sources = jnp.arange(TOK_DEV * TOP, dtype=jnp.int32) // TOP
    slot_table = jnp.full((EXPERTS * CAP,), -1, jnp.int32).at[target].set(sources)
    slot_weight = jnp.zeros((EXPERTS * CAP,), jnp.float32).at[target].set(block_weights.reshape(-1))
    return (slot_table, slot_weight)

def reference(resid, query, keys, values, q_gain, k_gain, out_weight, norm_gain, route_ids, route_weight, expert_gate, expert_up, expert_down):
    places = jnp.arange(LEN, dtype=jnp.int32)

    def one_sequence(operands):
        query_rows, key_rows, value_rows = operands
        query_turned = prepare(query_rows, q_gain, QH, places)
        key_turned = prepare(key_rows, k_gain, KVH, places)
        mixed = attend(query_turned, key_turned, value_rows.reshape(LEN, KVH, HD))
        return mixed.reshape(LEN, QH * HD)
    head_out = lax.map(one_sequence, (query, keys, values))
    projected = jnp.dot(head_out.reshape(SEQS * LEN, QH * HD), out_weight, preferred_element_type=jnp.float32)
    updated = (resid.reshape(SEQS * LEN, D).astype(jnp.float32) + projected).astype(jnp.bfloat16)
    widened = updated.astype(jnp.float32)
    normed = (widened * lax.rsqrt(lax.optimization_barrier(jnp.mean(widened * widened, axis=-1, keepdims=True)) + EPSILON) * norm_gain).astype(jnp.bfloat16)
    block_count = N_SP * N_DP
    slot_table, slot_weight = jax.vmap(block_tables)(route_ids.reshape(block_count, TOK_DEV, TOP), route_weight.reshape(block_count, TOK_DEV, TOP))
    slot_table = jnp.transpose(slot_table.reshape(block_count, EXPERTS, CAP), (1, 0, 2))
    slot_weight = jnp.transpose(slot_weight.reshape(block_count, EXPERTS, CAP), (1, 0, 2))
    block_start = (jnp.arange(block_count, dtype=jnp.int32) * TOK_DEV)[:, None]

    def one_expert(running, operands):
        gate_matrix, up_matrix, down_matrix, table_rows, weight_rows = operands
        valid = table_rows >= 0
        global_rows = jnp.where(valid, table_rows + block_start, 0).reshape(-1).astype(jnp.int32)
        answered = apply_expert(normed[global_rows], gate_matrix, up_matrix, down_matrix)
        scaled = answered.astype(jnp.float32) * jnp.where(valid, weight_rows, 0.0).reshape(-1)[:, None]
        return (running.at[global_rows].add(scaled), None)
    combined = lax.scan(one_expert, jnp.zeros((SEQS * LEN, D), jnp.float32), (expert_gate, expert_up, expert_down, slot_table, slot_weight))[0]
    return (widened + combined).astype(jnp.bfloat16).reshape(SEQS, LEN, D)
```

```python
import functools

import jax
import jax.numpy as jnp
from jax import lax
from jax.experimental import pallas as pl
from jax.experimental.pallas import tpu as pltpu
from jax.sharding import PartitionSpec as P

GRID_W = 64
EPSILON = 1e-06
THETA = 10000.0
LIMIT = 7.0
SLOPE = 1.702
LOG2E = 1.4426950408889634
MESH = pl.DeviceIdType.MESH
VMEM_BYTES = 64000000


def split_of(count, inner):
    return (count // inner, inner) if count % inner == 0 else (count, 1)


def turn_tables(places, head_dim):
    quarter = head_dim // 4
    inverse = THETA ** (-jnp.arange(quarter, dtype=jnp.float32) / quarter)
    row = (places // GRID_W).astype(jnp.float32)[:, None] * inverse[None, :]
    col = (places % GRID_W).astype(jnp.float32)[:, None] * inverse[None, :]
    cosine = jnp.concatenate([jnp.cos(row)] * 2 + [jnp.cos(col)] * 2, axis=-1)
    sine = jnp.concatenate(
        [-jnp.sin(row), jnp.sin(row), -jnp.sin(col), jnp.sin(col)], axis=-1
    )
    return cosine, sine


def attention_kernel(
    planes, lanes_x, outer_dp, inner_dp,
    q_ref, k_ref, v_ref, qg_ref, kg_ref, cos_ref, sin_ref, resid_ref, ng_ref, w_ref,
    upd_ref, normed_ref,
    kall, vall, wall, qt, acc, mx, ls, head_out,
    kx_s, kx_r, kz_s, kz_r, vz_s, vz_r, vx_s, vx_r, wy_s, wy_r, wc_s, wc_r, loc,
):
    Z, X, Y, C = planes, lanes_x, outer_dp, inner_dp
    rows, head_dim = cos_ref.shape
    q_heads = q_ref.shape[1] // head_dim
    kv_heads = k_ref.shape[1] // head_dim
    group = q_heads // kv_heads
    w_rows = w_ref.shape[0]
    sp, dp = lax.axis_index("sp"), lax.axis_index("dp")
    z, x = sp // X, sp % X
    y, c = dp // C, dp % C
    up_ok, down_ok = z + 1 < Z, z > 0

    barrier = pltpu.get_barrier_semaphore()

    def greet(device):
        pl.semaphore_signal(barrier, inc=1, device_id=device, device_id_type=MESH)

    for j in range(1, X):
        greet((z * X + (x + j) % X, dp))

    @pl.when(up_ok)
    def _():
        greet((sp + X, dp))

    @pl.when(down_ok)
    def _():
        greet((sp - X, dp))

    for j in range(1, Y):
        greet((sp, ((y + j) % Y) * C + c))
    for j in range(1, C):
        greet((sp, y * C + (c + j) % C))

    def krows(block):
        return pl.ds(pl.multiple_of(block * rows, rows), rows)

    def wrows(block):
        return pl.ds(pl.multiple_of(block * w_rows, w_rows), w_rows)

    v_own = pltpu.make_async_copy(v_ref, vall.at[krows(sp)], loc.at[0])
    v_own.start()
    w_own = pltpu.make_async_copy(w_ref, wall.at[wrows(dp)], loc.at[1])
    w_own.start()

    lane = lax.broadcasted_iota(jnp.int32, (rows, head_dim), 1)
    first = lane % (head_dim // 2) < head_dim // 4

    def turned(value, gain):
        value = value.astype(jnp.float32)
        value = value * lax.rsqrt(jnp.mean(value * value, axis=-1, keepdims=True) + EPSILON) * gain
        swapped = jnp.where(
            first,
            pltpu.roll(value, head_dim - head_dim // 4, 1),
            pltpu.roll(value, head_dim // 4, 1),
        )
        return (value * cos_ref[...] + swapped * sin_ref[...]).astype(jnp.bfloat16)

    for g in range(kv_heads):
        span = slice(g * head_dim, (g + 1) * head_dim)
        kall[krows(sp), span] = turned(k_ref[:, span], kg_ref[...])

    count = (X - 1) + (Y - 1) + (C - 1) + up_ok.astype(jnp.int32) + down_ok.astype(jnp.int32)
    v_own.wait()
    w_own.wait()
    pl.semaphore_wait(barrier, count)

    def remote(buf, sl, ssem, rsem, device):
        return pltpu.make_async_remote_copy(
            src_ref=buf.at[sl], dst_ref=buf.at[sl], send_sem=ssem, recv_sem=rsem,
            device_id=device, device_id_type=MESH,
        )

    def kx(j):
        return remote(kall, krows(sp), kx_s.at[j], kx_r.at[j], (z * X + (x + j) % X, dp))

    def kz(d, s, j):
        plane = z - s if d == 0 else z + s
        device = (sp + X if d == 0 else sp - X, dp)
        at = (d * (Z - 1) + s) * X + j
        return remote(kall, krows(plane * X + (x + X - j) % X), kz_s.at[at], kz_r.at[at], device)

    def vz(d, s):
        plane = z - s if d == 0 else z + s
        device = (sp + X if d == 0 else sp - X, dp)
        at = d * (Z - 1) + s
        return remote(vall, krows(plane * X + x), vz_s.at[at], vz_r.at[at], device)

    def vx(slot, plane, j):
        at = slot * X + j
        return remote(
            vall, krows(plane * X + x), vx_s.at[at], vx_r.at[at], (z * X + (x + j) % X, dp)
        )

    def sends(d, s):
        if d == 0:
            return jnp.logical_and(up_ok, z - s >= 0)
        return jnp.logical_and(down_ok, z + s < Z)

    def gets(d, s):
        return z - s - 1 >= 0 if d == 0 else z + s + 1 < Z

    def wy(j):
        return remote(wall, wrows(dp), wy_s.at[j], wy_r.at[j], (sp, ((y + j) % Y) * C + c))

    def wc(j, i):
        at = j * C + i
        return remote(
            wall, wrows(((y + Y - j) % Y) * C + c), wc_s.at[at], wc_r.at[at],
            (sp, y * C + (c + i) % C),
        )

    for j in range(1, X):
        kx(j).start()
    for d in range(2):
        @pl.when(sends(d, 0))
        def _(d=d):
            kz(d, 0, 0).start()
            vz(d, 0).start()
    for j in range(1, X):
        vx(0, z, j).start()
    for j in range(1, Y):
        wy(j).start()
    for i in range(1, C):
        wc(0, i).start()

    def prepare_queries(h, carry):
        at = pl.ds(pl.multiple_of(h * head_dim, head_dim), head_dim)
        qt[h] = turned(q_ref[:, at], qg_ref[...])
        return carry

    lax.fori_loop(0, q_heads // 4, prepare_queries, 0)
    for j in range(1, X):
        kx(j).wait_recv()
    for d in range(2):
        @pl.when(sends(d, 0))
        def _(d=d):
            for j in range(1, X):
                kz(d, 0, j).start()
    lax.fori_loop(q_heads // 4, q_heads, prepare_queries, 0)

    factor = head_dim ** (-0.5) * LOG2E
    keys_in = X * rows

    def attend(plane, fresh):
        at_rows = pl.ds(pl.multiple_of(plane * keys_in, keys_in), keys_in)

        def pair(i, carry):
            for u in range(2):
                h = i * 2 + u
                span = pl.ds(pl.multiple_of((h // group) * head_dim, head_dim), head_dim)
                scores = lax.dot_general(
                    qt[h], kall[at_rows, span], (((1,), (1,)), ((), ())),
                    preferred_element_type=jnp.float32,
                )
                top = jnp.max(scores, axis=-1, keepdims=True)
                if not fresh:
                    before = mx[h]
                    top = jnp.maximum(before[:, :1], top)
                lifted = jnp.exp2((scores - top) * factor)
                total = jnp.sum(lifted, axis=-1, keepdims=True)
                part = jnp.dot(
                    lifted.astype(jnp.bfloat16), vall[at_rows, span],
                    preferred_element_type=jnp.float32,
                )
                wide = jnp.broadcast_to(top, (rows, head_dim))
                wide_total = jnp.broadcast_to(total, (rows, head_dim))
                if fresh:
                    acc[h], ls[h] = part, wide_total
                else:
                    fade = jnp.exp2((before - wide) * factor)
                    acc[h] = acc[h] * fade + part
                    ls[h] = ls[h] * fade + wide_total
                mx[h] = wide
            return carry

        lax.fori_loop(0, q_heads // 2, pair, 0)

    def wait_vx(slot, plane):
        for j in range(1, X):
            vx(slot, plane, j).wait_recv()

    def attend_step(s):
        def one(t, carry):
            plane = jnp.where(t == 0, z - s - 1, z + s + 1)

            @pl.when(jnp.logical_and(plane >= 0, plane < Z))
            def _():
                wait_vx(1 + s + t * (Z - 1), plane)
                attend(plane, False)
            return carry

        lax.fori_loop(0, 2, one, 0)

    for s in range(Z - 1):
        for d in range(2):
            @pl.when(gets(d, s))
            def _(d=d, s=s):
                plane = z - s - 1 if d == 0 else z + s + 1
                vz(d, s).wait_recv()
                for j in range(1, X):
                    vx(1 + s + d * (Z - 1), plane, j).start()
                if s + 1 < Z - 1:
                    @pl.when(sends(d, s + 1))
                    def _():
                        vz(d, s + 1).start()
                for j in range(X):
                    kz(d, s, j).wait_recv()
                    if s + 1 < Z - 1:
                        @pl.when(sends(d, s + 1))
                        def _(j=j):
                            kz(d, s + 1, j).start()
        if s == 0:
            wait_vx(0, z)
            attend(z, True)
        else:
            attend_step(s - 1)
        if s == 0:
            pass
    if Z == 1:
        wait_vx(0, z)
        attend(z, True)
    else:
        attend_step(Z - 2)

    for j in range(1, Y):
        wy(j).wait_recv()
        for i in range(1, C):
            wc(j, i).start()

    for h in range(q_heads):
        head_out[:, h * head_dim:(h + 1) * head_dim] = (acc[h] / ls[h]).astype(jnp.bfloat16)

    for j in range(Y):
        for i in range(1, C):
            wc(j, i).wait_recv()

    width = wall.shape[1]
    tile = min(256, width)

    def project(n, total):
        at = pl.ds(pl.multiple_of(n * tile, tile), tile)
        projected = jnp.dot(head_out[...], wall[:, at], preferred_element_type=jnp.float32)
        updated = (resid_ref[:, at].astype(jnp.float32) + projected).astype(jnp.bfloat16)
        upd_ref[:, at] = updated
        wide = updated.astype(jnp.float32)
        return total + jnp.sum(wide * wide, axis=-1, keepdims=True)

    square = lax.fori_loop(0, width // tile, project, jnp.zeros((rows, 1), jnp.float32))
    scale = lax.rsqrt(square / width + EPSILON)

    def normalize(n, carry):
        at = pl.ds(pl.multiple_of(n * tile, tile), tile)
        normed_ref[:, at] = (
            upd_ref[:, at].astype(jnp.float32) * scale * ng_ref[:, at]
        ).astype(jnp.bfloat16)
        return carry

    lax.fori_loop(0, width // tile, normalize, 0)

    for j in range(1, X):
        kx(j).wait_send()
        vx(0, z, j).wait_send()
    for d in range(2):
        for s in range(Z - 1):
            @pl.when(sends(d, s))
            def _(d=d, s=s):
                vz(d, s).wait_send()
                for j in range(X):
                    kz(d, s, j).wait_send()

            @pl.when(gets(d, s))
            def _(d=d, s=s):
                plane = z - s - 1 if d == 0 else z + s + 1
                for j in range(1, X):
                    vx(1 + s + d * (Z - 1), plane, j).wait_send()
    for j in range(1, Y):
        wy(j).wait_send()
    for j in range(Y):
        for i in range(1, C):
            wc(j, i).wait_send()


def attention(query, keys, values, q_gain, k_gain, cosine, sine, resid, norm_gain, out_weight):
    sp_count, dp_count = lax.axis_size("sp"), lax.axis_size("dp")
    planes = 4 if sp_count % 4 == 0 else 1
    lanes_x = sp_count // planes
    outer_dp, inner_dp = split_of(dp_count, 2)
    rows, head_dim = cosine.shape
    q_heads = query.shape[1] // head_dim
    width = resid.shape[1]
    dma = pltpu.SemaphoreType.DMA
    vmem = pl.BlockSpec(memory_space=pltpu.VMEM)
    hops = 2 * max(planes - 1, 1)
    full_kv = (sp_count * rows, keys.shape[1])
    return pl.pallas_call(
        functools.partial(attention_kernel, planes, lanes_x, outer_dp, inner_dp),
        name="gathered_attention",
        out_shape=(
            jax.ShapeDtypeStruct((rows, width), jnp.bfloat16),
            jax.ShapeDtypeStruct((rows, width), jnp.bfloat16),
        ),
        in_specs=[vmem, vmem, pl.BlockSpec(memory_space=pl.ANY)]
        + [vmem] * 6
        + [pl.BlockSpec(memory_space=pl.ANY)],
        out_specs=(vmem, vmem),
        scratch_shapes=[
            pltpu.VMEM(full_kv, jnp.bfloat16),
            pltpu.VMEM(full_kv, jnp.bfloat16),
            pltpu.VMEM((dp_count * out_weight.shape[0], width), jnp.bfloat16),
            pltpu.VMEM((q_heads, rows, head_dim), jnp.bfloat16),
            pltpu.VMEM((q_heads, rows, head_dim), jnp.float32),
            pltpu.VMEM((q_heads, rows, head_dim), jnp.float32),
            pltpu.VMEM((q_heads, rows, head_dim), jnp.float32),
            pltpu.VMEM((rows, q_heads * head_dim), jnp.bfloat16),
            dma((lanes_x,)), dma((lanes_x,)),
            dma((hops * lanes_x,)), dma((hops * lanes_x,)),
            dma((hops,)), dma((hops,)),
            dma(((hops + 1) * lanes_x,)), dma(((hops + 1) * lanes_x,)),
            dma((outer_dp,)), dma((outer_dp,)),
            dma((outer_dp * inner_dp,)), dma((outer_dp * inner_dp,)),
            dma((2,)),
        ],
        compiler_params=pltpu.CompilerParams(
            collective_id=0, has_side_effects=True, vmem_limit_bytes=VMEM_BYTES
        ),
    )(
        query, keys, values, q_gain[None], k_gain[None], cosine, sine, resid,
        norm_gain[None], out_weight,
    )


def apply_expert(batch, gate_matrix, up_matrix, down_matrix):
    flat_rows = batch.reshape(-1, batch.shape[-1])
    gated = jnp.minimum(jnp.dot(flat_rows, gate_matrix, preferred_element_type=jnp.float32), LIMIT)
    linear = jnp.clip(
        jnp.dot(flat_rows, up_matrix, preferred_element_type=jnp.float32), -LIMIT, LIMIT
    )
    active = (gated * jax.nn.sigmoid(SLOPE * gated) * (linear + 1.0)).astype(jnp.bfloat16)
    return (
        jnp.dot(active, down_matrix, preferred_element_type=jnp.float32)
        .astype(jnp.bfloat16)
        .reshape(batch.shape)
    )


def per_device(
    resid,
    query,
    keys,
    values,
    q_gain,
    k_gain,
    out_weight,
    norm_gain,
    route_ids,
    route_weight,
    expert_gate,
    expert_up,
    expert_down,
):
    span_devices = lax.axis_size("sp")
    experts_total = span_devices * lax.axis_size("dp")
    tok_rows = resid.shape[1]
    model_width = resid.shape[2]
    head_dim = q_gain.shape[0]
    places = lax.axis_index("sp") * tok_rows + jnp.arange(tok_rows, dtype=jnp.int32)
    cosine, sine = turn_tables(places, head_dim)
    updated, normed = attention(
        query[0], keys[0], values[0], q_gain, k_gain, cosine, sine, resid[0], norm_gain, out_weight
    )
    widened = updated.astype(jnp.float32)
    top_count = route_ids.shape[2]
    capacity = max(2, 3 * tok_rows * top_count // (2 * experts_total))
    chosen = route_ids[0].reshape(-1)
    onehot = (chosen[:, None] == jnp.arange(experts_total, dtype=jnp.int32)[None, :]).astype(
        jnp.int32
    )
    earlier = jnp.sum((jnp.cumsum(onehot, axis=0) - onehot) * onehot, axis=1)
    target = chosen * capacity + earlier
    sources = jnp.arange(tok_rows * top_count, dtype=jnp.int32) // top_count
    slot_table = jnp.full((experts_total * capacity,), tok_rows, jnp.int32).at[target].set(sources)
    padded = jnp.concatenate([normed, jnp.zeros((1, model_width), jnp.bfloat16)], axis=0)
    outgoing = padded[slot_table].reshape(experts_total, capacity, model_width)
    answered = apply_expert(
        lax.all_to_all(outgoing, ("sp", "dp"), split_axis=0, concat_axis=0, tiled=True),
        expert_gate[0],
        expert_up[0],
        expert_down[0],
    )
    returned = lax.all_to_all(answered, ("sp", "dp"), split_axis=0, concat_axis=0, tiled=True)
    results = returned.reshape(experts_total * capacity, model_width)[target]
    weighted = results.astype(jnp.float32) * route_weight[0].reshape(-1)[:, None]
    combined = jnp.sum(weighted.reshape(tok_rows, top_count, model_width), axis=1)
    return (widened + combined).astype(jnp.bfloat16)[None]


def solution(mesh):
    placed = (
        P("dp", "sp", None),
        P("dp", "sp", None),
        P("dp", "sp", None),
        P("dp", "sp", None),
        P(),
        P(),
        P("dp", None),
        P(),
        P("dp", "sp", None),
        P("dp", "sp", None),
        P(("sp", "dp"), None, None),
        P(("sp", "dp"), None, None),
        P(("sp", "dp"), None, None),
    )
    return jax.shard_map(
        per_device, mesh=mesh, in_specs=placed, out_specs=P("dp", "sp", None), check_vma=False
    )
```

```python
import functools

import jax
import jax.numpy as jnp
from jax import lax
from jax.experimental import pallas as pl
from jax.experimental.pallas import tpu as pltpu
from jax.sharding import PartitionSpec as P

GRID_W = 64
EPSILON = 1e-06
THETA = 10000.0
LIMIT = 7.0
SLOPE = 1.702
LOG2E = 1.4426950408889634
MESH = pl.DeviceIdType.MESH
VMEM_BYTES = 64000000


def split_of(count, inner):
    return (count // inner, inner) if count % inner == 0 else (count, 1)


def turn_tables(places, head_dim):
    quarter = head_dim // 4
    inverse = THETA ** (-jnp.arange(quarter, dtype=jnp.float32) / quarter)
    row = (places // GRID_W).astype(jnp.float32)[:, None] * inverse[None, :]
    col = (places % GRID_W).astype(jnp.float32)[:, None] * inverse[None, :]
    cosine = jnp.concatenate([jnp.cos(row)] * 2 + [jnp.cos(col)] * 2, axis=-1)
    sine = jnp.concatenate(
        [-jnp.sin(row), jnp.sin(row), -jnp.sin(col), jnp.sin(col)], axis=-1
    )
    return cosine, sine


def attention_kernel(
    planes, lanes_x, outer_dp, inner_dp,
    q_ref, k_ref, v_ref, qg_ref, kg_ref, cos_ref, sin_ref, resid_ref, ng_ref, w_ref,
    upd_ref, normed_ref,
    kall, vall, wall, qt, acc, mx, ls, head_out,
    kx_s, kx_r, kz_s, kz_r, vz_s, vz_r, vx_s, vx_r, wy_s, wy_r, wc_s, wc_r, loc,
):
    Z, X, Y, C = planes, lanes_x, outer_dp, inner_dp
    rows, head_dim = cos_ref.shape
    q_heads = q_ref.shape[1] // head_dim
    kv_heads = k_ref.shape[1] // head_dim
    group = q_heads // kv_heads
    w_rows = w_ref.shape[0]
    sp, dp = lax.axis_index("sp"), lax.axis_index("dp")
    z, x = sp // X, sp % X
    y, c = dp // C, dp % C
    up_ok, down_ok = z + 1 < Z, z > 0

    barrier = pltpu.get_barrier_semaphore()

    def greet(device):
        pl.semaphore_signal(barrier, inc=1, device_id=device, device_id_type=MESH)

    for j in range(1, X):
        greet((z * X + (x + j) % X, dp))

    @pl.when(up_ok)
    def _():
        greet((sp + X, dp))

    @pl.when(down_ok)
    def _():
        greet((sp - X, dp))

    for j in range(1, Y):
        greet((sp, ((y + j) % Y) * C + c))
    for j in range(1, C):
        greet((sp, y * C + (c + j) % C))

    def krows(block):
        return pl.ds(pl.multiple_of(block * rows, rows), rows)

    def wrows(block):
        return pl.ds(pl.multiple_of(block * w_rows, w_rows), w_rows)

    v_own = pltpu.make_async_copy(v_ref, vall.at[krows(sp)], loc.at[0])
    v_own.start()
    w_own = pltpu.make_async_copy(w_ref, wall.at[wrows(dp)], loc.at[1])
    w_own.start()

    lane = lax.broadcasted_iota(jnp.int32, (rows, head_dim), 1)
    first = lane % (head_dim // 2) < head_dim // 4

    def turned(value, gain):
        value = value.astype(jnp.float32)
        value = value * lax.rsqrt(jnp.mean(value * value, axis=-1, keepdims=True) + EPSILON) * gain
        swapped = jnp.where(
            first,
            pltpu.roll(value, head_dim - head_dim // 4, 1),
            pltpu.roll(value, head_dim // 4, 1),
        )
        return (value * cos_ref[...] + swapped * sin_ref[...]).astype(jnp.bfloat16)

    for g in range(kv_heads):
        span = slice(g * head_dim, (g + 1) * head_dim)
        kall[krows(sp), span] = turned(k_ref[:, span], kg_ref[...])

    count = (X - 1) + (Y - 1) + (C - 1) + up_ok.astype(jnp.int32) + down_ok.astype(jnp.int32)
    v_own.wait()
    w_own.wait()
    pl.semaphore_wait(barrier, count)

    def remote(buf, sl, ssem, rsem, device):
        return pltpu.make_async_remote_copy(
            src_ref=buf.at[sl], dst_ref=buf.at[sl], send_sem=ssem, recv_sem=rsem,
            device_id=device, device_id_type=MESH,
        )

    def kx(j):
        return remote(kall, krows(sp), kx_s.at[j], kx_r.at[j], (z * X + (x + j) % X, dp))

    def kz(d, s, j):
        plane = z - s if d == 0 else z + s
        device = (sp + X if d == 0 else sp - X, dp)
        at = (d * (Z - 1) + s) * X + j
        return remote(kall, krows(plane * X + (x + X - j) % X), kz_s.at[at], kz_r.at[at], device)

    def vz(d, s):
        plane = z - s if d == 0 else z + s
        device = (sp + X if d == 0 else sp - X, dp)
        at = d * (Z - 1) + s
        return remote(vall, krows(plane * X + x), vz_s.at[at], vz_r.at[at], device)

    def vx(slot, plane, j):
        at = slot * X + j
        return remote(
            vall, krows(plane * X + x), vx_s.at[at], vx_r.at[at], (z * X + (x + j) % X, dp)
        )

    def sends(d, s):
        if d == 0:
            return jnp.logical_and(up_ok, z - s >= 0)
        return jnp.logical_and(down_ok, z + s < Z)

    def gets(d, s):
        return z - s - 1 >= 0 if d == 0 else z + s + 1 < Z

    def wy(j):
        return remote(wall, wrows(dp), wy_s.at[j], wy_r.at[j], (sp, ((y + j) % Y) * C + c))

    def wc(j, i):
        at = j * C + i
        return remote(
            wall, wrows(((y + Y - j) % Y) * C + c), wc_s.at[at], wc_r.at[at],
            (sp, y * C + (c + i) % C),
        )

    for j in range(1, X):
        kx(j).start()
    for d in range(2):
        @pl.when(sends(d, 0))
        def _(d=d):
            kz(d, 0, 0).start()
            vz(d, 0).start()
    for j in range(1, X):
        vx(0, z, j).start()
    for j in range(1, Y):
        wy(j).start()
    for i in range(1, C):
        wc(0, i).start()

    def prepare_queries(h, carry):
        at = pl.ds(pl.multiple_of(h * head_dim, head_dim), head_dim)
        qt[h] = turned(q_ref[:, at], qg_ref[...])
        return carry

    lax.fori_loop(0, q_heads // 4, prepare_queries, 0)
    for j in range(1, X):
        kx(j).wait_recv()
    for d in range(2):
        @pl.when(sends(d, 0))
        def _(d=d):
            for j in range(1, X):
                kz(d, 0, j).start()
    lax.fori_loop(q_heads // 4, q_heads, prepare_queries, 0)

    factor = head_dim ** (-0.5) * LOG2E
    keys_in = X * rows

    def attend(plane, fresh):
        at_rows = pl.ds(pl.multiple_of(plane * keys_in, keys_in), keys_in)

        def one_group(i, carry):
            span = pl.ds(pl.multiple_of(i * head_dim, head_dim), head_dim)
            for u in range(group):
                h = i * group + u
                scores = lax.dot_general(
                    qt[h], kall[at_rows, span], (((1,), (1,)), ((), ())),
                    preferred_element_type=jnp.float32,
                )
                top = jnp.max(scores, axis=-1, keepdims=True)
                if not fresh:
                    before = mx[h]
                    top = jnp.maximum(before[:, :1], top)
                lifted = jnp.exp2((scores - top) * factor)
                total = jnp.sum(lifted, axis=-1, keepdims=True)
                part = jnp.dot(
                    lifted.astype(jnp.bfloat16), vall[at_rows, span],
                    preferred_element_type=jnp.float32,
                )
                wide = jnp.broadcast_to(top, (rows, head_dim))
                wide_total = jnp.broadcast_to(total, (rows, head_dim))
                if fresh:
                    acc[h], ls[h] = part, wide_total
                else:
                    fade = jnp.exp2((before - wide) * factor)
                    acc[h] = acc[h] * fade + part
                    ls[h] = ls[h] * fade + wide_total
                mx[h] = wide
            return carry

        lax.fori_loop(0, kv_heads, one_group, 0)

    def wait_vx(slot, plane):
        for j in range(1, X):
            vx(slot, plane, j).wait_recv()

    def attend_step(s):
        def one(t, carry):
            plane = jnp.where(t == 0, z - s - 1, z + s + 1)

            @pl.when(jnp.logical_and(plane >= 0, plane < Z))
            def _():
                wait_vx(1 + s + t * (Z - 1), plane)
                attend(plane, False)
            return carry

        lax.fori_loop(0, 2, one, 0)

    for s in range(Z - 1):
        for d in range(2):
            @pl.when(gets(d, s))
            def _(d=d, s=s):
                plane = z - s - 1 if d == 0 else z + s + 1
                vz(d, s).wait_recv()
                for j in range(1, X):
                    vx(1 + s + d * (Z - 1), plane, j).start()
                if s + 1 < Z - 1:
                    @pl.when(sends(d, s + 1))
                    def _():
                        vz(d, s + 1).start()
                for j in range(X):
                    kz(d, s, j).wait_recv()
                    if s + 1 < Z - 1:
                        @pl.when(sends(d, s + 1))
                        def _(j=j):
                            kz(d, s + 1, j).start()
        if s == 0:
            wait_vx(0, z)
            attend(z, True)
        else:
            attend_step(s - 1)

    for j in range(1, Y):
        wy(j).wait_recv()
        for i in range(1, C):
            wc(j, i).start()
    if Z == 1:
        wait_vx(0, z)
        attend(z, True)
    else:
        attend_step(Z - 2)

    for h in range(q_heads):
        head_out[:, h * head_dim:(h + 1) * head_dim] = (acc[h] / ls[h]).astype(jnp.bfloat16)

    for j in range(Y):
        for i in range(1, C):
            wc(j, i).wait_recv()

    width = wall.shape[1]
    tile = min(256, width)

    def project(n, total):
        at = pl.ds(pl.multiple_of(n * tile, tile), tile)
        projected = jnp.dot(head_out[...], wall[:, at], preferred_element_type=jnp.float32)
        updated = (resid_ref[:, at].astype(jnp.float32) + projected).astype(jnp.bfloat16)
        upd_ref[:, at] = updated
        wide = updated.astype(jnp.float32)
        return total + jnp.sum(wide * wide, axis=-1, keepdims=True)

    square = lax.fori_loop(0, width // tile, project, jnp.zeros((rows, 1), jnp.float32))
    scale = lax.rsqrt(square / width + EPSILON)

    def normalize(n, carry):
        at = pl.ds(pl.multiple_of(n * tile, tile), tile)
        normed_ref[:, at] = (
            upd_ref[:, at].astype(jnp.float32) * scale * ng_ref[:, at]
        ).astype(jnp.bfloat16)
        return carry

    lax.fori_loop(0, width // tile, normalize, 0)

    for j in range(1, X):
        kx(j).wait_send()
        vx(0, z, j).wait_send()
    for d in range(2):
        for s in range(Z - 1):
            @pl.when(sends(d, s))
            def _(d=d, s=s):
                vz(d, s).wait_send()
                for j in range(X):
                    kz(d, s, j).wait_send()

            @pl.when(gets(d, s))
            def _(d=d, s=s):
                plane = z - s - 1 if d == 0 else z + s + 1
                for j in range(1, X):
                    vx(1 + s + d * (Z - 1), plane, j).wait_send()
    for j in range(1, Y):
        wy(j).wait_send()
    for j in range(Y):
        for i in range(1, C):
            wc(j, i).wait_send()


def attention(query, keys, values, q_gain, k_gain, cosine, sine, resid, norm_gain, out_weight):
    sp_count, dp_count = lax.axis_size("sp"), lax.axis_size("dp")
    planes = 4 if sp_count % 4 == 0 else 1
    lanes_x = sp_count // planes
    outer_dp, inner_dp = split_of(dp_count, 2)
    rows, head_dim = cosine.shape
    q_heads = query.shape[1] // head_dim
    width = resid.shape[1]
    dma = pltpu.SemaphoreType.DMA
    vmem = pl.BlockSpec(memory_space=pltpu.VMEM)
    hops = 2 * max(planes - 1, 1)
    full_kv = (sp_count * rows, keys.shape[1])
    return pl.pallas_call(
        functools.partial(attention_kernel, planes, lanes_x, outer_dp, inner_dp),
        name="gathered_attention",
        out_shape=(
            jax.ShapeDtypeStruct((rows, width), jnp.bfloat16),
            jax.ShapeDtypeStruct((rows, width), jnp.bfloat16),
        ),
        in_specs=[vmem, vmem, pl.BlockSpec(memory_space=pl.ANY)]
        + [vmem] * 6
        + [pl.BlockSpec(memory_space=pl.ANY)],
        out_specs=(vmem, vmem),
        scratch_shapes=[
            pltpu.VMEM(full_kv, jnp.bfloat16),
            pltpu.VMEM(full_kv, jnp.bfloat16),
            pltpu.VMEM((dp_count * out_weight.shape[0], width), jnp.bfloat16),
            pltpu.VMEM((q_heads, rows, head_dim), jnp.bfloat16),
            pltpu.VMEM((q_heads, rows, head_dim), jnp.float32),
            pltpu.VMEM((q_heads, rows, head_dim), jnp.float32),
            pltpu.VMEM((q_heads, rows, head_dim), jnp.float32),
            pltpu.VMEM((rows, q_heads * head_dim), jnp.bfloat16),
            dma((lanes_x,)), dma((lanes_x,)),
            dma((hops * lanes_x,)), dma((hops * lanes_x,)),
            dma((hops,)), dma((hops,)),
            dma(((hops + 1) * lanes_x,)), dma(((hops + 1) * lanes_x,)),
            dma((outer_dp,)), dma((outer_dp,)),
            dma((outer_dp * inner_dp,)), dma((outer_dp * inner_dp,)),
            dma((2,)),
        ],
        compiler_params=pltpu.CompilerParams(
            collective_id=0, has_side_effects=True, vmem_limit_bytes=VMEM_BYTES
        ),
    )(
        query, keys, values, q_gain[None], k_gain[None], cosine, sine, resid,
        norm_gain[None], out_weight,
    )


def apply_expert(batch, gate_matrix, up_matrix, down_matrix):
    flat_rows = batch.reshape(-1, batch.shape[-1])
    gated = jnp.minimum(jnp.dot(flat_rows, gate_matrix, preferred_element_type=jnp.float32), LIMIT)
    linear = jnp.clip(
        jnp.dot(flat_rows, up_matrix, preferred_element_type=jnp.float32), -LIMIT, LIMIT
    )
    active = (gated * jax.nn.sigmoid(SLOPE * gated) * (linear + 1.0)).astype(jnp.bfloat16)
    return (
        jnp.dot(active, down_matrix, preferred_element_type=jnp.float32)
        .astype(jnp.bfloat16)
        .reshape(batch.shape)
    )


def per_device(
    resid,
    query,
    keys,
    values,
    q_gain,
    k_gain,
    out_weight,
    norm_gain,
    route_ids,
    route_weight,
    expert_gate,
    expert_up,
    expert_down,
):
    span_devices = lax.axis_size("sp")
    experts_total = span_devices * lax.axis_size("dp")
    tok_rows = resid.shape[1]
    model_width = resid.shape[2]
    head_dim = q_gain.shape[0]
    places = lax.axis_index("sp") * tok_rows + jnp.arange(tok_rows, dtype=jnp.int32)
    cosine, sine = turn_tables(places, head_dim)
    updated, normed = attention(
        query[0], keys[0], values[0], q_gain, k_gain, cosine, sine, resid[0], norm_gain, out_weight
    )
    widened = updated.astype(jnp.float32)
    top_count = route_ids.shape[2]
    capacity = max(2, 3 * tok_rows * top_count // (2 * experts_total))
    chosen = route_ids[0].reshape(-1)
    onehot = (chosen[:, None] == jnp.arange(experts_total, dtype=jnp.int32)[None, :]).astype(
        jnp.int32
    )
    earlier = jnp.sum((jnp.cumsum(onehot, axis=0) - onehot) * onehot, axis=1)
    target = chosen * capacity + earlier
    sources = jnp.arange(tok_rows * top_count, dtype=jnp.int32) // top_count
    slot_table = jnp.full((experts_total * capacity,), tok_rows, jnp.int32).at[target].set(sources)
    padded = jnp.concatenate([normed, jnp.zeros((1, model_width), jnp.bfloat16)], axis=0)
    outgoing = padded[slot_table].reshape(experts_total, capacity, model_width)
    answered = apply_expert(
        lax.all_to_all(outgoing, ("sp", "dp"), split_axis=0, concat_axis=0, tiled=True),
        expert_gate[0],
        expert_up[0],
        expert_down[0],
    )
    returned = lax.all_to_all(answered, ("sp", "dp"), split_axis=0, concat_axis=0, tiled=True)
    rows_back = returned.reshape(experts_total * capacity, model_width)
    slots = target.reshape(tok_rows, top_count)
    combined = sum(
        rows_back[slots[:, i]].astype(jnp.float32) * route_weight[0, :, i][:, None]
        for i in range(top_count)
    )
    return (widened + combined).astype(jnp.bfloat16)[None]


def solution(mesh):
    placed = (
        P("dp", "sp", None),
        P("dp", "sp", None),
        P("dp", "sp", None),
        P("dp", "sp", None),
        P(),
        P(),
        P("dp", None),
        P(),
        P("dp", "sp", None),
        P("dp", "sp", None),
        P(("sp", "dp"), None, None),
        P(("sp", "dp"), None, None),
        P(("sp", "dp"), None, None),
    )
    return jax.shard_map(
        per_device, mesh=mesh, in_specs=placed, out_specs=P("dp", "sp", None), check_vma=False
    )
```
